32 devices in a mesh: ep: 8 (over z, core), tp: 4 (over y, x).
Axes of the slice: x: 2, y: 2, z: 4, core: 2. Of those that a mesh axis runs over, the one named last changes fastest.
Arguments:
- queries: bfloat16 [1024, 1536], P('ep', 'tp'), may hold values from -64 to 64
- kv_latent: bfloat16 [1024, 512], P('ep'), may hold values from -60 to 60
- rope_key: bfloat16 [1024, 32], P('ep'), may hold values from -64 to 64
- latent_gain: float32 [512], replicated, may hold values from 0.1 to 1.9
- key_up: bfloat16 [512, 1024], P(None, 'tp'), may hold values from -0.25 to 0.25
- value_up: bfloat16 [512, 1024], P(None, 'tp'), may hold values from -40 to 40
- query_gain: float32 [96], replicated, may hold values from 0.3 to 4
- key_gain: float32 [96], replicated, may hold values from 0.3 to 4
- out_gain: float32 [1024], replicated, may hold values from 0.1 to 1.9
- out_proj: bfloat16 [1024, 4096], P(None, 'tp'), may hold values from -0.1875 to 0.1875
- moe_input: bfloat16 [1024, 4096], P('ep'), may hold values from -60 to 60
- moe_gain: float32 [4096], replicated, may hold values from 0.1 to 1.9
- expert_ids: int32 [1024, 2], P('ep'), may hold values from 0 to 31, as said below
- route_weights: float32 [1024, 2], P('ep'), may hold values from 0.2 to 1
- w_gate: bfloat16 [32, 4096, 2048], P('ep', None, 'tp'), may hold values from -0.09375 to 0.09375
- w_up: bfloat16 [32, 4096, 2048], P('ep', None, 'tp'), may hold values from -0.09375 to 0.09375
- w_down: bfloat16 [32, 2048, 4096], P('ep', 'tp'), may hold values from -0.125 to 0.125
Outputs:
- mixed: bfloat16 [1024, 4096], P('ep', 'tp')
- expert_out: bfloat16 [1024, 4096], P('ep', 'tp')
The draws below stay inside these ranges and needn't reach their ends.
Inputs may be any that keep to these rules, and one draw needn't show every extreme that they name: `expert_ids`: both experts of a row lie in one group (g * 8 to g * 8 + 7) and differ. In each aligned block of 128 rows no expert is named more than 12 times, and some expert is named exactly 12 times.
All inputs are finite; a program needn't handle non-finite values.
Results may differ from the reference program's by a relative error of at most 0.015.
The reference program's roundings to bfloat16 on the way count: a program that leaves them out, or rounds other values in their place, can miss the bound.
Values may be sent and summed in bfloat16 or wider, within the bound.
A program may use at most 128 MiB of HBM per device.

```python
import jax
import jax.numpy as jnp
from jax import lax

D = 4096
HEADS = 16
NOPE = 64
ROPE = 32
VDIM = 64
KV_RANK = 512
PER_GROUP = 8
D_EXP = 2048
TOP = 2
TOK_DEV = 128
QKD = 96
EXPERTS = 32
TOKENS = 1024
CAP = 12
N_EP = 8
N_TP = 4


def draw_rope_key(key, part):
    drawn = jnp.clip(jax.random.normal(jax.random.fold_in(key, 21), (TOKENS, ROPE), jnp.float32), -6.0, 6.0)
    return drawn.astype(jnp.bfloat16)


def draw_queries(key, part):
    drawn = jnp.clip(jax.random.normal(jax.random.fold_in(key, 31), (TOKENS, HEADS, QKD), jnp.float32), -6.0, 6.0)
    return drawn.reshape(TOKENS, HEADS * QKD).astype(jnp.bfloat16)


def draw_query_gain(key, part):
    drawn = jax.random.uniform(jax.random.fold_in(key, 41), (QKD,), jnp.float32, 0.3, 1.7)
    return drawn


def draw_key_gain(key, part):
    drawn = jax.random.uniform(jax.random.fold_in(key, 51), (QKD,), jnp.float32, 0.3, 1.7)
    return drawn


def scaled_rows(key, salt, row_count, col_count):
    drawn = jnp.clip(jax.random.normal(jax.random.fold_in(key, salt), (row_count, col_count), jnp.float32), -6.0, 6.0)
    return drawn


def draw_kv_latent(key, part):
    return scaled_rows(key, 61, TOKENS, KV_RANK).astype(jnp.bfloat16)


def draw_moe_input(key, part):
    return scaled_rows(key, 71, TOKENS, D).astype(jnp.bfloat16)


def draw_value_up(key, part):
    drawn = jax.random.normal(jax.random.fold_in(key, 81), (KV_RANK, HEADS * VDIM), jnp.float32) * KV_RANK ** (-0.5)
    head_pos = (jnp.arange(HEADS * VDIM) // VDIM).astype(jnp.float32) / (HEADS - 1)
    scale = 3.0 ** head_pos
    return jnp.clip(drawn * scale[None, :], -40.0, 40.0).astype(jnp.bfloat16)


def draw_expert_ids(key, part):
    block_keys = jax.random.split(jax.random.fold_in(key, 91), TOKENS // TOK_DEV)

    def one_block(block_key):
        parts_key = jax.random.split(block_key, 6)
        biggest = jax.random.randint(parts_key[0], (), 0, 4)
        low_count = TOK_DEV // 8
        high_count = TOK_DEV // 4
        count_a = jax.random.randint(parts_key[1], (), low_count, high_count + 1)
        count_b = jax.random.randint(parts_key[2], (), low_count, high_count + 1)
        count_c = 5 * TOK_DEV // 8 - count_a - count_b
        others = (biggest + 1 + jnp.arange(3)) % 4
        counts = jnp.zeros((4,), jnp.int32).at[biggest].set(3 * TOK_DEV // 8)
        counts = counts.at[others].set(jnp.stack([count_a, count_b, count_c]).astype(jnp.int32))
        ends = jnp.cumsum(counts)
        ranks = jnp.arange(TOK_DEV)
        group_of = jnp.sum((ranks[:, None] >= ends[None, :]).astype(jnp.int32), axis=1)
        within = ranks - (ends - counts)[group_of]
        shifts = jax.random.randint(parts_key[3], (4,), 0, PER_GROUP)
        steps_apart = jax.random.randint(parts_key[4], (4,), 1, PER_GROUP)
        first_pick = (shifts[group_of] + within) % PER_GROUP
        second_pick = (shifts[group_of] + within + steps_apart[group_of]) % PER_GROUP
        chosen = jnp.stack([first_pick, second_pick], axis=1) + group_of[:, None] * PER_GROUP
        order = jax.random.permutation(parts_key[5], TOK_DEV)
        return chosen[order]
    return jax.vmap(one_block)(block_keys).reshape(TOKENS, 2).astype(jnp.int32)


def block_levels(own_key, shape, cuts, low, largest):
    factor_of, own = 1.0, jax.random.fold_in(own_key, 6)
    for dim, blocks in cuts:
        draws = jnp.exp(jax.random.uniform(jax.random.fold_in(own, dim), (blocks,), jnp.float32, low / len(cuts), largest / len(cuts)))
        factor_of = factor_of * jnp.repeat(draws, shape[dim] // blocks).reshape([-1 if axis == dim else 1 for axis in range(len(shape))])
    return factor_of


def noise(key, dims, deviation, most, cuts=(), kind=jnp.bfloat16):
    entries = jax.random.normal(key, dims, jnp.float32) * deviation
    if len(cuts) > 0:
        entries = block_levels(key, dims, cuts, -0.22, 0.18) * entries
    return jnp.clip(entries, min=-most, max=most).astype(kind)


def setup_inputs(seed: int = 0) -> dict:
    seeds = jax.random.split(jax.random.key(seed), 18)
    return {
        "queries": draw_queries(jax.random.fold_in(seeds[17], 71), 0),
        "kv_latent": draw_kv_latent(jax.random.fold_in(seeds[17], 71), 0),
        "rope_key": draw_rope_key(jax.random.fold_in(seeds[17], 71), 0),
        "latent_gain": jnp.clip(1.0 + 0.18 * jax.random.normal(seeds[3], (KV_RANK,), jnp.float32), 0.1, 1.9),
        "key_up": noise(seeds[4], (KV_RANK, HEADS * NOPE), KV_RANK ** -0.5, 0.25, ((1, 4),)),
        "value_up": draw_value_up(jax.random.fold_in(seeds[17], 71), 0),
        "query_gain": draw_query_gain(jax.random.fold_in(seeds[17], 71), 0),
        "key_gain": draw_key_gain(jax.random.fold_in(seeds[17], 71), 0),
        "out_gain": jnp.clip(1.0 + 0.18 * jax.random.normal(seeds[8], (HEADS * VDIM,), jnp.float32), 0.1, 1.9),
        "out_proj": noise(seeds[9], (HEADS * VDIM, D), (HEADS * VDIM) ** -0.5, 0.1875, ((1, 4),)),
        "moe_input": draw_moe_input(jax.random.fold_in(seeds[17], 71), 0),
        "moe_gain": jnp.clip(1.0 + 0.18 * jax.random.normal(seeds[11], (D,), jnp.float32), 0.1, 1.9),
        "expert_ids": draw_expert_ids(jax.random.fold_in(seeds[17], 71), 0),
        "route_weights": jnp.clip(0.2 + 0.8 * jax.random.uniform(seeds[13], (TOKENS, TOP), jnp.float32) ** block_levels(seeds[13], (TOKENS, TOP), ((0, 8),), -0.2, 0.2), 0.2, 1.0),
        "w_gate": noise(seeds[14], (EXPERTS, D, D_EXP), D ** -0.5, 0.09375, ((0, 8), (2, 4))),
        "w_up": noise(seeds[15], (EXPERTS, D, D_EXP), D ** -0.5, 0.09375, ((0, 8), (2, 4))),
        "w_down": noise(seeds[16], (EXPERTS, D_EXP, D), D_EXP ** -0.5, 0.125, ((0, 8), (1, 4))),
    }


EPS = 1e-06
THETA = 10000.0

def rotate_half(values_in, positions):
    half_width = ROPE // 2
    inverse = THETA ** (-jnp.arange(half_width, dtype=jnp.float32) / half_width)
    angles = positions.astype(jnp.float32)[:, None] * inverse
    cosine = jnp.cos(angles)[:, None, :]
    sine = jnp.sin(angles)[:, None, :]
    first_half = values_in[..., :half_width]
    second_half = values_in[..., half_width:]
    return jnp.concatenate([first_half * cosine - second_half * sine, second_half * cosine + first_half * sine], axis=-1)

def head_norm(values_in, gain_vec):
    return values_in * lax.rsqrt(lax.optimization_barrier(jnp.mean(values_in * values_in, axis=-1, keepdims=True)) + EPS) * gain_vec

def make_queries(queries, query_gain, positions):
    row_count = queries.shape[0]
    head_count = queries.shape[1] // QKD
    normed = head_norm(queries.astype(jnp.float32).reshape(row_count, head_count, QKD), query_gain)
    turned = jnp.concatenate([normed[..., :NOPE], rotate_half(normed[..., NOPE:], positions)], axis=-1)
    return turned.astype(jnp.bfloat16)

def make_keys(latent, rope_part, latent_gain, key_up, value_up, key_gain, positions):
    row_count = latent.shape[0]
    head_count = key_up.shape[1] // NOPE
    latent_f = latent.astype(jnp.float32)
    latent_n = (latent_f * lax.rsqrt(lax.optimization_barrier(jnp.mean(latent_f * latent_f, axis=-1, keepdims=True)) + EPS) * latent_gain).astype(jnp.bfloat16)
    key_nope = jnp.dot(latent_n, key_up, preferred_element_type=jnp.float32).astype(jnp.bfloat16)
    key_nope = lax.optimization_barrier(key_nope)
    value_rows = jnp.dot(latent_n, value_up, preferred_element_type=jnp.float32).astype(jnp.bfloat16)
    shared = jnp.broadcast_to(rope_part.astype(jnp.float32)[:, None, :], (row_count, head_count, ROPE))
    key_full = jnp.concatenate([key_nope.astype(jnp.float32).reshape(row_count, head_count, NOPE), shared], axis=-1)
    normed = head_norm(key_full, key_gain)
    turned = jnp.concatenate([normed[..., :NOPE], rotate_half(normed[..., NOPE:], positions)], axis=-1)
    return (turned.astype(jnp.bfloat16), value_rows.reshape(row_count, head_count, VDIM))

def attention(query_rot, key_rot, value_rows):
    block_rows = 512
    block_count = TOKENS // block_rows
    key_pos = jnp.arange(TOKENS)
    keys_f = key_rot.astype(jnp.float32)
    values_f = value_rows.astype(jnp.float32)
    head_count = query_rot.shape[1]

    def one_block(index):
        first = index * block_rows
        query_blk = lax.dynamic_slice_in_dim(query_rot, first, block_rows, 0).astype(jnp.float32)
        scores = jnp.einsum('qhd,khd->hqk', query_blk, keys_f) * QKD ** (-0.5)
        query_pos = first + jnp.arange(block_rows)
        visible = key_pos[None, :] <= query_pos[:, None]
        scores = jnp.where(visible[None], scores, -1e+30)
        top_score = lax.optimization_barrier(jnp.max(scores, axis=-1, keepdims=True))
        expo = jnp.exp(scores - top_score)
        probs = lax.optimization_barrier(expo.astype(jnp.bfloat16))
        totals = lax.optimization_barrier(jnp.sum(expo, axis=-1))
        weighted = jnp.einsum('hqk,khd->hqd', probs.astype(jnp.float32), values_f) / totals[..., None]
        return weighted.astype(jnp.bfloat16)
    outcome = lax.map(one_block, jnp.arange(block_count))
    return outcome.transpose(0, 2, 1, 3).reshape(TOKENS, head_count * VDIM)

def reference(queries, kv_latent, rope_key, latent_gain, key_up, value_up, query_gain, key_gain, out_gain, out_proj, moe_input, moe_gain, expert_ids, route_weights, w_gate, w_up, w_down):
    positions = jnp.arange(TOKENS, dtype=jnp.int32)
    query_rot = make_queries(queries, query_gain, positions)
    key_rot, value_rows = make_keys(kv_latent, rope_key, latent_gain, key_up, value_up, key_gain, positions)
    attn = attention(query_rot, key_rot, value_rows)
    attn_f = attn.astype(jnp.float32)
    inverse_rms = lax.rsqrt(lax.optimization_barrier(jnp.mean(attn_f * attn_f, axis=-1)) + EPS)
    attn_n = (attn_f * out_gain).astype(jnp.bfloat16)
    mixed = (jnp.dot(attn_n, out_proj, preferred_element_type=jnp.float32) * inverse_rms[:, None]).astype(jnp.bfloat16)
    stream_f = moe_input.astype(jnp.float32)
    normed = (stream_f * lax.rsqrt(lax.optimization_barrier(jnp.mean(stream_f * stream_f, axis=-1, keepdims=True)) + EPS) * moe_gain).astype(jnp.bfloat16)
    flat_ids = expert_ids.reshape(-1).astype(jnp.int32)
    pick_count = TOKENS * TOP
    onehot = (flat_ids[:, None] == jnp.arange(EXPERTS, dtype=jnp.int32)[None, :]).astype(jnp.int32)
    per_block = onehot.reshape(N_EP, TOK_DEV * TOP, EXPERTS)
    earlier = (jnp.cumsum(per_block, axis=1) - per_block).astype(jnp.int32)
    slot_rank = lax.optimization_barrier(jnp.sum(earlier * per_block, axis=-1)).reshape(-1).astype(jnp.int32)
    block_index = (jnp.arange(pick_count, dtype=jnp.int32) // (TOK_DEV * TOP)).astype(jnp.int32)
    slot_count = N_EP * CAP
    slot_index = (flat_ids * slot_count + block_index * CAP + slot_rank).astype(jnp.int32)
    token_index = (jnp.arange(pick_count, dtype=jnp.int32) // TOP).astype(jnp.int32)
    slot_token = jnp.zeros((EXPERTS * slot_count,), jnp.int32).at[slot_index].set(token_index)
    expert_rows = normed[slot_token].reshape(EXPERTS, slot_count, D)
    shard_width = D_EXP // N_TP

    def one_expert(operands):
        rows_in, gate_w, up_w, down_w = operands
        gate = jnp.dot(rows_in, gate_w, preferred_element_type=jnp.float32)
        upper = jnp.dot(rows_in, up_w, preferred_element_type=jnp.float32)
        act = (jax.nn.silu(gate) * upper).astype(jnp.bfloat16)
        partials = jnp.einsum('sjf,jfd->jsd', act.reshape(slot_count, N_TP, shard_width).astype(jnp.float32), down_w.reshape(N_TP, shard_width, D).astype(jnp.float32))
        partials = lax.optimization_barrier(partials.astype(jnp.bfloat16))
        return lax.optimization_barrier(jnp.sum(partials.astype(jnp.float32), axis=0)).astype(jnp.bfloat16)
    expert_y = lax.map(one_expert, (expert_rows, w_gate, w_up, w_down)).reshape(EXPERTS * slot_count, D)
    picked = expert_y[slot_index].reshape(TOKENS, TOP, D).astype(jnp.float32)
    expert_out = lax.optimization_barrier(jnp.sum(picked * route_weights[..., None], axis=1)).astype(jnp.bfloat16)
    return (mixed, expert_out)
```

```python
import functools

import jax
import jax.numpy as jnp
from jax import lax
from jax.experimental import pallas as pl
from jax.experimental.pallas import tpu as pltpu
from jax.sharding import PartitionSpec as P

NOPE = 64
ROPE = 32
VDIM = 64
QKD = 96
CAP = 12


EPS = 1e-06
THETA = 10000.0


def rotate_half(values_in, positions):
    half_width = ROPE // 2
    inverse = THETA ** (-jnp.arange(half_width, dtype=jnp.float32) / half_width)
    angles = positions.astype(jnp.float32)[:, None] * inverse
    cosine = jnp.cos(angles)[:, None, :]
    sine = jnp.sin(angles)[:, None, :]
    first_half = values_in[..., :half_width]
    second_half = values_in[..., half_width:]
    return jnp.concatenate(
        [first_half * cosine - second_half * sine, second_half * cosine + first_half * sine],
        axis=-1,
    )


def head_norm(values_in, gain_vec):
    return (
        values_in
        * lax.rsqrt(jnp.mean(values_in * values_in, axis=-1, keepdims=True) + EPS)
        * gain_vec
    )


def make_queries(queries, query_gain, positions):
    row_count = queries.shape[0]
    head_count = queries.shape[1] // QKD
    normed = head_norm(queries.astype(jnp.float32).reshape(row_count, head_count, QKD), query_gain)
    turned = jnp.concatenate(
        [normed[..., :NOPE], rotate_half(normed[..., NOPE:], positions)], axis=-1
    )
    return turned.astype(jnp.bfloat16)


def make_keys(latent, rope_part, latent_gain, key_up, value_up, key_gain, positions):
    row_count = latent.shape[0]
    head_count = key_up.shape[1] // NOPE
    latent_f = latent.astype(jnp.float32)
    latent_n = (
        latent_f
        * lax.rsqrt(jnp.mean(latent_f * latent_f, axis=-1, keepdims=True) + EPS)
        * latent_gain
    ).astype(jnp.bfloat16)
    key_nope = jnp.dot(latent_n, key_up, preferred_element_type=jnp.float32).astype(jnp.bfloat16)
    key_nope = lax.optimization_barrier(key_nope)
    value_rows = jnp.dot(latent_n, value_up, preferred_element_type=jnp.float32).astype(
        jnp.bfloat16
    )
    shared = jnp.broadcast_to(
        rope_part.astype(jnp.float32)[:, None, :], (row_count, head_count, ROPE)
    )
    key_full = jnp.concatenate(
        [key_nope.astype(jnp.float32).reshape(row_count, head_count, NOPE), shared], axis=-1
    )
    normed = head_norm(key_full, key_gain)
    turned = jnp.concatenate(
        [normed[..., :NOPE], rotate_half(normed[..., NOPE:], positions)], axis=-1
    )
    return (turned.astype(jnp.bfloat16), value_rows.reshape(row_count, head_count, VDIM))


def shards(
    queries,
    kv_latent,
    rope_key,
    latent_gain,
    key_up,
    value_up,
    query_gain,
    key_gain,
    out_gain,
    out_proj,
    moe_input,
    moe_gain,
    expert_ids,
    route_weights,
    w_gate,
    w_up,
    w_down,
):
    tok_rows = queries.shape[0]
    head_count = key_up.shape[1] // NOPE
    query_pos = lax.axis_index("ep") * tok_rows + jnp.arange(tok_rows, dtype=jnp.int32)
    query_rot = make_queries(queries, query_gain, query_pos)
    inv_scale = QKD ** (-0.5)
    blocks_in = (
        lax.all_gather(kv_latent, "ep", axis=0, tiled=True),
        lax.all_gather(rope_key, "ep", axis=0, tiled=True),
    )
    key_pos = jnp.arange(blocks_in[0].shape[0], dtype=jnp.int32)
    key_rot, value_rows = make_keys(
        blocks_in[0], blocks_in[1], latent_gain, key_up, value_up, key_gain, key_pos
    )
    top_prev = jnp.full((head_count, tok_rows), -1e30, jnp.float32)
    key_pos = jnp.arange(key_rot.shape[0], dtype=jnp.int32)
    scores = (
        jnp.einsum("qhd,khd->hqk", query_rot, key_rot, preferred_element_type=jnp.float32)
        * inv_scale
    )
    visible = key_pos[None, :] <= query_pos[:, None]
    scores = jnp.where(visible[None], scores, -1e30)
    top_new = jnp.maximum(top_prev, jnp.max(scores, axis=-1))
    expo = jnp.exp(scores - top_new[..., None])
    total_new = jnp.sum(expo, axis=-1)
    accum_new = jnp.einsum(
        "hqk,khd->hqd", expo.astype(jnp.bfloat16), value_rows, preferred_element_type=jnp.float32
    )
    attn = (accum_new / total_new[..., None]).astype(jnp.bfloat16)
    attn = attn.transpose(1, 0, 2).reshape(tok_rows, head_count * VDIM)
    block_f = lax.all_gather(attn, "tp", axis=1, tiled=True).astype(jnp.float32)
    scaled = (block_f * out_gain[None, :]).astype(jnp.bfloat16)
    product = jnp.dot(scaled, out_proj, preferred_element_type=jnp.float32)
    product, squares = (product, jnp.sum(block_f * block_f, axis=-1))
    mixed = (product * lax.rsqrt(squares / out_gain.shape[0] + EPS)[:, None]).astype(jnp.bfloat16)
    row_count = moe_input.shape[0]
    top_count = expert_ids.shape[1]
    local_experts = w_gate.shape[0]
    ep_count = lax.axis_size("ep")
    expert_count = local_experts * ep_count
    stream_f = moe_input.astype(jnp.float32)
    normed = (
        stream_f * lax.rsqrt(jnp.mean(stream_f * stream_f, axis=-1, keepdims=True) + EPS) * moe_gain
    ).astype(jnp.bfloat16)
    flat_ids = expert_ids.reshape(-1)
    onehot = (flat_ids[:, None] == jnp.arange(expert_count, dtype=jnp.int32)[None, :]).astype(
        jnp.int32
    )
    slot_rank = jnp.sum((jnp.cumsum(onehot, axis=0) - onehot) * onehot, axis=1)
    slot_index = flat_ids * CAP + slot_rank
    token_index = jnp.arange(row_count * top_count, dtype=jnp.int32) // top_count
    slot_token = jnp.zeros((expert_count * CAP,), jnp.int32).at[slot_index].set(token_index)
    slot_used = jnp.zeros((expert_count * CAP,), jnp.bool_).at[slot_index].set(True)
    outgoing = jnp.where(slot_used[:, None], normed[slot_token], jnp.zeros((), jnp.bfloat16))
    outgoing = outgoing.reshape(ep_count, local_experts, CAP, normed.shape[1])
    piece_width = normed.shape[1] // lax.axis_size("tp")
    my_columns = lax.dynamic_slice_in_dim(
        outgoing, lax.axis_index("tp") * piece_width, piece_width, 3
    )
    arrived_part = lax.all_to_all(my_columns, "ep", split_axis=0, concat_axis=0, tiled=True)
    piece = lax.all_gather(arrived_part, "tp", axis=3, tiled=True)
    gate_acc = jnp.einsum("secd,edf->secf", piece, w_gate, preferred_element_type=jnp.float32)
    upper_acc = jnp.einsum("secd,edf->secf", piece, w_up, preferred_element_type=jnp.float32)
    hidden = (jax.nn.silu(gate_acc) * upper_acc).astype(jnp.bfloat16)
    out_cols = w_down.shape[2] // lax.axis_size("tp")
    term = jnp.einsum("secf,efd->dsec", hidden, w_down, preferred_element_type=jnp.float32)
    summed = lax.psum_scatter(
        term.reshape(lax.axis_size("tp") * out_cols, -1).astype(jnp.bfloat16),
        "tp",
        scatter_dimension=0,
        tiled=True,
    )
    expert_y = summed.T.reshape(ep_count, local_experts * CAP, out_cols)
    returned_rows = lax.all_to_all(expert_y, "ep", split_axis=0, concat_axis=0, tiled=True).reshape(
        expert_count * CAP, out_cols
    )
    picked = returned_rows[slot_index].reshape(row_count, top_count, out_cols).astype(jnp.float32)
    expert_out = jnp.sum(picked * route_weights[..., None], axis=1).astype(jnp.bfloat16)
    return (mixed, expert_out)


MESH = pl.DeviceIdType.MESH
GROUP = 8
PAD = 128


def group_cap():
    return GROUP * CAP // 2


def rdma(src, dst, send_sem, recv_sem, device):
    copy = pltpu.make_async_remote_copy(
        src_ref=src,
        dst_ref=dst,
        send_sem=send_sem,
        recv_sem=recv_sem,
        device_id=device,
        device_id_type=MESH,
    )
    copy.start()
    return copy


def arrived(dst, sem, device):
    pltpu.make_async_remote_copy(
        src_ref=dst,
        dst_ref=dst,
        send_sem=sem,
        recv_sem=sem,
        device_id=device,
        device_id_type=MESH,
    ).wait_recv()


def places(planes):
    ep = lax.axis_index("ep")
    tp = lax.axis_index("tp")
    plane = ep // 2
    core = ep % 2

    def along(offset):
        return (lax.rem(plane + offset + planes, planes) * 2 + core, tp)

    partner = (plane * 2 + 1 - core, tp)
    near_x = (ep, tp ^ 1)
    near_y = (ep, tp ^ 2)
    corner = (ep, tp ^ 3)
    return tp, along, partner, near_x, near_y, corner


def greet(peers):
    barrier = pltpu.get_barrier_semaphore()
    for peer in peers:
        pl.semaphore_signal(barrier, inc=1, device_id=peer, device_id_type=MESH)
    pl.semaphore_wait(barrier, len(peers))


def dispatch_kernel(
    planes,
    out_ref,
    meta_ref,
    kv_ref,
    rows_ref,
    metas_ref,
    keys_ref,
    zs,
    zr,
    xs,
    xr,
    ps,
    pr,
    loc,
):
    tp, along, partner, near_x, near_y, _ = places(planes)
    greet([along(d) for d in range(1, planes)] + [partner, near_x, near_y])
    half_w = out_ref.shape[2] // 2
    half_r = kv_ref.shape[0] // 2
    sent = []
    local = [
        pltpu.make_async_copy(kv_ref, keys_ref.at[tp, 0, 0], loc.at[0]),
        pltpu.make_async_copy(meta_ref.at[0], metas_ref.at[0, 0], loc.at[1]),
        pltpu.make_async_copy(out_ref.at[0], rows_ref.at[tp, 0, 0], loc.at[2]),
    ]
    for copy in local:
        copy.start()
    for d in range(1, planes):
        sent.append(rdma(kv_ref, keys_ref.at[tp, 0, d], zs.at[0, d], zr.at[0, d], along(d)))
    for d in range(1, planes):
        sent.append(
            rdma(meta_ref.at[d], metas_ref.at[0, d], zs.at[1, d], zr.at[1, d], along(d))
        )
        sent.append(
            rdma(out_ref.at[d], rows_ref.at[tp, 0, d], zs.at[2, d], zr.at[2, d], along(d))
        )
    for copy in local:
        copy.wait()
    bufs = (keys_ref, rows_ref)

    def halves(kind, ref):
        if kind == 0:
            return ref.at[pl.ds(0, half_r)], ref.at[pl.ds(half_r, half_r)]
        return ref.at[:, pl.ds(0, half_w)], ref.at[:, pl.ds(half_w, half_w)]

    def to_partner(kind, which, q, d):
        sent.append(
            rdma(
                bufs[kind].at[q, 0, d],
                bufs[kind].at[q, 1, d],
                ps.at[kind, which, d],
                pr.at[kind, which, d],
                partner,
            )
        )

    def first(kind, d):
        mine = bufs[kind].at[tp, 0, d]
        if d > 0:
            arrived(mine, zr.at[2 * kind, d], along(-d))
        sent.append(rdma(mine, mine, xs.at[kind, 0, d], xr.at[kind, 0, d], near_x))
        sent.append(rdma(mine, mine, xs.at[kind, 1, d], xr.at[kind, 1, d], near_y))
        to_partner(kind, 0, tp, d)
        if kind == 1:
            part = metas_ref.at[0, d]
            if d > 0:
                arrived(part, zr.at[1, d], along(-d))
            sent.append(rdma(part, metas_ref.at[1, d], ps.at[2, 0, d], pr.at[2, 0, d], partner))

    def second(kind, d):
        from_x = bufs[kind].at[tp ^ 1, 0, d]
        arrived(from_x, xr.at[kind, 0, d], near_x)
        low, _ = halves(kind, from_x)
        sent.append(rdma(low, low, xs.at[kind, 2, d], xr.at[kind, 2, d], near_y))
        from_y = bufs[kind].at[tp ^ 2, 0, d]
        arrived(from_y, xr.at[kind, 1, d], near_y)
        _, high = halves(kind, from_y)
        sent.append(rdma(high, high, xs.at[kind, 3, d], xr.at[kind, 3, d], near_x))
        to_partner(kind, 1, tp ^ 1, d)
        to_partner(kind, 2, tp ^ 2, d)

    def third(kind, d):
        low, high = halves(kind, bufs[kind].at[tp ^ 3, 0, d])
        arrived(low, xr.at[kind, 2, d], near_y)
        arrived(high, xr.at[kind, 3, d], near_x)
        to_partner(kind, 3, tp ^ 3, d)

    jobs = [(0, d) for d in range(planes)] + [(1, d) for d in range(planes)]
    for step in range(len(jobs) + 4):
        if step < len(jobs):
            first(*jobs[step])
        if 0 <= step - 2 < len(jobs):
            second(*jobs[step - 2])
        if 0 <= step - 4 < len(jobs):
            third(*jobs[step - 4])
    for d in range(planes):
        for kind in range(2):
            for which, flip in enumerate((0, 1, 2, 3)):
                arrived(bufs[kind].at[tp ^ flip, 1, d], pr.at[kind, which, d], partner)
        arrived(metas_ref.at[1, d], pr.at[2, 0, d], partner)
    for copy in sent:
        copy.wait_send()


def dispatch(outgoing, metas, kv_part, tp_count):
    planes, cap, width = outgoing.shape
    dma = pltpu.SemaphoreType.DMA
    return pl.pallas_call(
        functools.partial(dispatch_kernel, planes),
        out_shape=(
            jax.ShapeDtypeStruct((tp_count, 2, planes, cap, width), jnp.bfloat16),
            jax.ShapeDtypeStruct((2, planes, cap, PAD), jnp.bfloat16),
            jax.ShapeDtypeStruct((tp_count, 2, planes) + kv_part.shape, jnp.bfloat16),
        ),
        in_specs=[pl.BlockSpec(memory_space=pltpu.VMEM)] * 3,
        out_specs=(pl.BlockSpec(memory_space=pltpu.VMEM),) * 3,
        scratch_shapes=[
            dma((3, planes)),
            dma((3, planes)),
            dma((2, 4, planes)),
            dma((2, 4, planes)),
            dma((3, 4, planes)),
            dma((3, 4, planes)),
            dma((3,)),
        ],
        compiler_params=pltpu.CompilerParams(
            collective_id=0, has_side_effects=True, vmem_limit_bytes=40 * 2**20
        ),
        name="dispatch",
    )(outgoing, metas, kv_part)


def expert_kernel(
    pick_ref, place_ref, weight_ref, rows_ref, gate_ref, up_ref, down_ref, out_ref, g_acc, u_acc, total
):
    expert = pl.program_id(0)
    quarter = pl.program_id(1)
    experts = pl.num_programs(0)
    quarters = pl.num_programs(1)

    picked = jnp.dot(
        pick_ref[...], rows_ref[quarter], preferred_element_type=jnp.float32
    ).astype(jnp.bfloat16)
    gate = jnp.dot(picked, gate_ref[...], preferred_element_type=jnp.float32)
    upper = jnp.dot(picked, up_ref[...], preferred_element_type=jnp.float32)

    @pl.when(quarter == 0)
    def _():
        g_acc[...] = gate
        u_acc[...] = upper

    @pl.when(quarter > 0)
    def _():
        g_acc[...] += gate
        u_acc[...] += upper

    @pl.when(quarter == quarters - 1)
    def _():
        g = g_acc[...]
        hidden = (g / (1.0 + jnp.exp(-g)) * u_acc[...] * weight_ref[...]).astype(jnp.bfloat16)
        blocks, parts, cap, width = out_ref.shape
        for q in range(parts):
            y = jnp.dot(
                hidden, down_ref[:, q * width : (q + 1) * width], preferred_element_type=jnp.float32
            ).astype(jnp.bfloat16)
            back = jnp.dot(place_ref[...], y, preferred_element_type=jnp.float32)

            @pl.when(expert == 0)
            def _():
                total[q] = back

            @pl.when(expert > 0)
            def _():
                total[q] += back

            @pl.when(expert == experts - 1)
            def _():
                out_ref[:, q] = total[q].reshape(blocks, cap, width).astype(jnp.bfloat16)


def run_experts(pick, place, weights, rows, w_gate, w_up, w_down, blocks, cap):
    experts, slots, row_count = pick.shape
    parts, _, width = rows.shape
    hidden = w_gate.shape[2]
    return pl.pallas_call(
        expert_kernel,
        grid=(experts, parts),
        out_shape=jax.ShapeDtypeStruct((blocks, parts, cap, width), jnp.bfloat16),
        in_specs=[
            pl.BlockSpec((None, slots, row_count), lambda e, q: (e, 0, 0)),
            pl.BlockSpec((None, row_count, slots), lambda e, q: (e, 0, 0)),
            pl.BlockSpec((None, slots, 1), lambda e, q: (e, 0, 0)),
            pl.BlockSpec((parts, row_count, width), lambda e, q: (0, 0, 0)),
            pl.BlockSpec((None, width, hidden), lambda e, q: (e, q, 0)),
            pl.BlockSpec((None, width, hidden), lambda e, q: (e, q, 0)),
            pl.BlockSpec((None, hidden, parts * width), lambda e, q: (e, 0, 0)),
        ],
        out_specs=pl.BlockSpec((blocks, parts, cap, width), lambda e, q: (0, 0, 0, 0)),
        scratch_shapes=[
            pltpu.VMEM((slots, hidden), jnp.float32),
            pltpu.VMEM((slots, hidden), jnp.float32),
            pltpu.VMEM((parts, row_count, width), jnp.float32),
        ],
        compiler_params=pltpu.CompilerParams(
            dimension_semantics=("arbitrary", "arbitrary"), vmem_limit_bytes=56 * 2**20
        ),
        name="experts",
    )(pick, place, weights, rows, w_gate, w_up, w_down)


def combine_kernel(
    planes,
    part_ref,
    attn_ref,
    back_ref,
    heads_ref,
    other,
    sums,
    bx1,
    by1,
    bx2,
    by2,
    done,
    as_,
    ar,
    ps,
    pr,
    xs,
    xr,
    zs,
    zr,
    loc,
):
    tp, along, partner, near_x, near_y, corner = places(planes)
    greet([along(d) for d in range(1, planes)] + [partner, near_x, near_y, corner])
    half_w = part_ref.shape[4] // 2
    low, high = pl.ds(0, half_w), pl.ds(half_w, half_w)
    sent = []
    order = list(range(1, planes)) + [0]
    for d in order:
        sent.append(rdma(part_ref.at[1, d], other.at[d], ps.at[d], pr.at[d], partner))
    own = pltpu.make_async_copy(attn_ref, heads_ref.at[tp], loc.at[0])
    own.start()
    for i, peer in enumerate((near_x, near_y, corner)):
        sent.append(rdma(attn_ref, heads_ref.at[tp], as_.at[i], ar.at[i], peer))

    def first(d):
        arrived(other.at[d], pr.at[d], partner)
        for q in range(part_ref.shape[2]):
            sums[d, q] = (
                part_ref[0, d, q].astype(jnp.float32) + other[d, q].astype(jnp.float32)
            ).astype(jnp.bfloat16)
        piece = sums.at[d, tp ^ 3]
        sent.append(rdma(piece.at[:, low], bx1.at[d], xs.at[0, d], xr.at[0, d], near_x))
        sent.append(rdma(piece.at[:, high], by1.at[d], xs.at[1, d], xr.at[1, d], near_y))

    def second(d):
        arrived(bx1.at[d], xr.at[0, d], near_x)
        sums[d, tp ^ 2, :, low] = (
            sums[d, tp ^ 2, :, low].astype(jnp.float32) + bx1[d].astype(jnp.float32)
        ).astype(jnp.bfloat16)
        sent.append(rdma(sums.at[d, tp ^ 2], by2.at[d], xs.at[3, d], xr.at[3, d], near_y))
        arrived(by1.at[d], xr.at[1, d], near_y)
        sums[d, tp ^ 1, :, high] = (
            sums[d, tp ^ 1, :, high].astype(jnp.float32) + by1[d].astype(jnp.float32)
        ).astype(jnp.bfloat16)
        sent.append(rdma(sums.at[d, tp ^ 1], bx2.at[d], xs.at[2, d], xr.at[2, d], near_x))

    def third(d):
        arrived(bx2.at[d], xr.at[2, d], near_x)
        arrived(by2.at[d], xr.at[3, d], near_y)
        full = (
            sums[d, tp].astype(jnp.float32)
            + bx2[d].astype(jnp.float32)
            + by2[d].astype(jnp.float32)
        ).astype(jnp.bfloat16)
        if d == 0:
            back_ref[0] = full
        else:
            done[d] = full
            sent.append(rdma(done.at[d], back_ref.at[d], zs.at[d], zr.at[d], along(-d)))

    for step in range(planes + 2):
        if step < planes:
            first(order[step])
        if 0 <= step - 1 < planes:
            second(order[step - 1])
        if 0 <= step - 2 < planes:
            third(order[step - 2])
    own.wait()
    for i, peer in enumerate((near_x, near_y, corner)):
        arrived(heads_ref.at[tp ^ (i + 1)], ar.at[i], peer)
    for d in range(1, planes):
        arrived(back_ref.at[d], zr.at[d], along(d))
    for copy in sent:
        copy.wait_send()


def combine(parts, attn):
    _, planes, tp_count, cap, width = parts.shape
    dma = pltpu.SemaphoreType.DMA
    bf = jnp.bfloat16
    return pl.pallas_call(
        functools.partial(combine_kernel, planes),
        out_shape=(
            jax.ShapeDtypeStruct((planes, cap, width), bf),
            jax.ShapeDtypeStruct((tp_count,) + attn.shape, bf),
        ),
        in_specs=[pl.BlockSpec(memory_space=pltpu.VMEM)] * 2,
        out_specs=(pl.BlockSpec(memory_space=pltpu.VMEM),) * 2,
        scratch_shapes=[
            pltpu.VMEM((planes, tp_count, cap, width), bf),
            pltpu.VMEM((planes, tp_count, cap, width), bf),
            pltpu.VMEM((planes, cap, width // 2), bf),
            pltpu.VMEM((planes, cap, width // 2), bf),
            pltpu.VMEM((planes, cap, width), bf),
            pltpu.VMEM((planes, cap, width), bf),
            pltpu.VMEM((planes, cap, width), bf),
            dma((3,)),
            dma((3,)),
            dma((planes,)),
            dma((planes,)),
            dma((4, planes)),
            dma((4, planes)),
            dma((planes,)),
            dma((planes,)),
            dma((1,)),
        ],
        compiler_params=pltpu.CompilerParams(
            collective_id=1, has_side_effects=True, vmem_limit_bytes=40 * 2**20
        ),
        name="combine",
    )(parts, attn)


def grouped_shards(
    queries,
    kv_latent,
    rope_key,
    latent_gain,
    key_up,
    value_up,
    query_gain,
    key_gain,
    out_gain,
    out_proj,
    moe_input,
    moe_gain,
    expert_ids,
    route_weights,
    w_gate,
    w_up,
    w_down,
):
    f32, bf = jnp.float32, jnp.bfloat16
    ep, tp = lax.axis_index("ep"), lax.axis_index("tp")
    tp_count = lax.axis_size("tp")
    planes = lax.axis_size("ep") // 2
    plane, core = ep // 2, ep % 2
    tokens, model = moe_input.shape
    width = model // tp_count
    local_experts = w_gate.shape[0]
    cap = group_cap()
    blocks = 2 * planes

    group = expert_ids[:, 0] // GROUP
    offset = lax.rem(group - plane + planes, planes)
    before = (jnp.arange(tokens)[:, None] > jnp.arange(tokens)[None, :]).astype(bf)
    in_group = offset[:, None] == jnp.arange(planes)[None, :]
    local_ids = expert_ids % GROUP
    hit = [offset[:, None] * GROUP + local_ids[:, k : k + 1] == jnp.arange(planes * GROUP)[None, :] for k in range(2)]
    counted = jnp.concatenate([in_group, hit[0] | hit[1]], axis=1).astype(bf)
    earlier = jnp.dot(before, counted, preferred_element_type=f32)
    rank = jnp.sum(jnp.where(in_group, earlier[:, :planes], 0.0), axis=1).astype(jnp.int32)
    codes = [
        local_ids[:, k].astype(f32) * CAP
        + jnp.sum(jnp.where(hit[k], earlier[:, planes:], 0.0), axis=1)
        + 1.0
        for k in range(2)
    ]
    weight_high = lax.reduce_precision(route_weights, 8, 7)
    weight_low = route_weights - weight_high
    meta = jnp.concatenate(
        [codes[0][:, None], codes[1][:, None], weight_high, weight_low], axis=1
    ).astype(bf)
    meta = jnp.pad(meta, ((0, 0), (0, PAD - meta.shape[1])))
    slot = offset * cap + rank
    select = (jnp.arange(planes * cap)[:, None] == slot[None, :]).astype(bf)

    stream_f = moe_input.astype(f32)
    scale = lax.rsqrt(jnp.mean(stream_f * stream_f, axis=-1, keepdims=True) + EPS)
    own_cols = lax.dynamic_slice_in_dim(moe_input, tp * width, width, 1).astype(f32)
    own_gain = lax.dynamic_slice_in_dim(moe_gain, tp * width, width, 0)
    normed = (own_cols * scale * own_gain).astype(bf)
    outgoing = jnp.dot(select, normed, preferred_element_type=f32).astype(bf)
    metas_out = jnp.dot(select, meta, preferred_element_type=f32).astype(bf)

    kv_rows = kv_latent.shape[0] // tp_count
    kv_all = jnp.pad(
        jnp.concatenate([kv_latent, rope_key], axis=1), ((0, 0), (0, PAD - ROPE))
    )
    kv_part = lax.dynamic_slice_in_dim(kv_all, tp * kv_rows, kv_rows, 0)
    rows, metas, keys = dispatch(
        outgoing.reshape(planes, cap, width), metas_out.reshape(planes, cap, PAD), kv_part, tp_count
    )

    row_total = blocks * cap
    slots = blocks * CAP
    info = metas.reshape(row_total, PAD)[:, :6].astype(f32)
    block_of = jnp.arange(row_total, dtype=jnp.int32) // cap
    positions = []
    for k in range(2):
        code = info[:, k].astype(jnp.int32) - 1 - core * (local_experts * CAP)
        inside = (info[:, k] > 0.5) & (code >= 0) & (code < local_experts * CAP)
        where = (code // CAP) * slots + block_of * CAP + code % CAP
        positions.append(jnp.where(inside, where, -1))
    slot_ids = jnp.arange(local_experts * slots, dtype=jnp.int32).reshape(local_experts, slots)
    match = [slot_ids[:, :, None] == positions[k][None, None, :] for k in range(2)]
    pick = (match[0] | match[1]).astype(bf)
    flip = [slot_ids[:, None, :] == positions[k][None, :, None] for k in range(2)]
    place = (flip[0] | flip[1]).astype(bf)
    weight_of = [info[:, 2 + k] + info[:, 4 + k] for k in range(2)]
    weights = jnp.sum(
        jnp.where(match[0], weight_of[0][None, None, :], 0.0)
        + jnp.where(match[1], weight_of[1][None, None, :], 0.0),
        axis=2,
        keepdims=True,
    )
    partial = run_experts(
        pick,
        place,
        weights,
        rows.reshape(tp_count, row_total, width),
        w_gate,
        w_up,
        w_down,
        blocks,
        cap,
    ).reshape(2, planes, tp_count, cap, width)

    tok_rows = queries.shape[0]
    head_count = key_up.shape[1] // NOPE
    query_pos = ep * tok_rows + jnp.arange(tok_rows, dtype=jnp.int32)
    query_rot = make_queries(queries, query_gain, query_pos)
    latent_width = kv_latent.shape[1]
    key_table = keys.reshape(-1, keys.shape[-1])
    quarter = jnp.arange(tp_count, dtype=jnp.int32)[:, None, None, None]
    parity = jnp.arange(2, dtype=jnp.int32)[None, :, None, None]
    away = jnp.arange(planes, dtype=jnp.int32)[None, None, :, None]
    key_block = lax.rem(plane - away + planes, planes) * 2 + lax.rem(core + parity, 2)
    key_pos = (
        key_block * tok_rows
        + quarter * kv_rows
        + jnp.arange(kv_rows, dtype=jnp.int32)[None, None, None, :]
    ).reshape(-1)
    key_rot, value_rows = make_keys(
        key_table[:, :latent_width],
        key_table[:, latent_width : latent_width + ROPE],
        latent_gain,
        key_up,
        value_up,
        key_gain,
        key_pos,
    )
    scores = (
        jnp.einsum("qhd,khd->hqk", query_rot, key_rot, preferred_element_type=f32) * QKD ** (-0.5)
    )
    visible = key_pos[None, :] <= query_pos[:, None]
    scores = jnp.where(visible[None], scores, -1e30)
    expo = jnp.exp(scores - jnp.max(scores, axis=-1, keepdims=True))
    total = jnp.sum(expo, axis=-1)
    accum = jnp.einsum("hqk,khd->hqd", expo.astype(bf), value_rows, preferred_element_type=f32)
    attn = (accum / total[..., None]).astype(bf)
    attn = attn.transpose(1, 0, 2).reshape(tok_rows, head_count * VDIM)

    returned, heads = combine(partial, attn)

    block_f = heads.transpose(1, 0, 2).reshape(tok_rows, -1).astype(f32)
    scaled = (block_f * out_gain[None, :]).astype(bf)
    product = jnp.dot(scaled, out_proj, preferred_element_type=f32)
    squares = jnp.sum(block_f * block_f, axis=-1)
    mixed = (product * lax.rsqrt(squares / out_gain.shape[0] + EPS)[:, None]).astype(bf)
    expert_out = lax.dot_general(
        select,
        returned.reshape(planes * cap, width),
        (((0,), (0,)), ((), ())),
        preferred_element_type=f32,
    ).astype(bf)
    return (mixed, expert_out)


def layer(*arrays):
    local_experts = arrays[14].shape[0]
    fits = lax.axis_size("tp") == 4 and 2 * local_experts == GROUP
    return grouped_shards(*arrays) if fits else shards(*arrays)


def solution(mesh):
    in_specs = (
        P("ep", "tp"),
        P("ep", None),
        P("ep", None),
        P(),
        P(None, "tp"),
        P(None, "tp"),
        P(),
        P(),
        P(),
        P(None, "tp"),
        P("ep", None),
        P(),
        P("ep", None),
        P("ep", None),
        P("ep", None, "tp"),
        P("ep", None, "tp"),
        P("ep", "tp", None),
    )
    out_specs = (P("ep", "tp"), P("ep", "tp"))
    return jax.shard_map(layer, mesh=mesh, in_specs=in_specs, out_specs=out_specs, check_vma=False)
```

```python
import functools

import jax
import jax.numpy as jnp
from jax import lax
from jax.experimental import pallas as pl
from jax.experimental.pallas import tpu as pltpu
from jax.sharding import PartitionSpec as P

NOPE = 64
ROPE = 32
VDIM = 64
QKD = 96
CAP = 12


EPS = 1e-06
THETA = 10000.0


def rotate_half(values_in, positions):
    half_width = ROPE // 2
    inverse = THETA ** (-jnp.arange(half_width, dtype=jnp.float32) / half_width)
    angles = positions.astype(jnp.float32)[:, None] * inverse
    cosine = jnp.cos(angles)[:, None, :]
    sine = jnp.sin(angles)[:, None, :]
    first_half = values_in[..., :half_width]
    second_half = values_in[..., half_width:]
    return jnp.concatenate(
        [first_half * cosine - second_half * sine, second_half * cosine + first_half * sine],
        axis=-1,
    )


def head_norm(values_in, gain_vec):
    return (
        values_in
        * lax.rsqrt(jnp.mean(values_in * values_in, axis=-1, keepdims=True) + EPS)
        * gain_vec
    )


def make_queries(queries, query_gain, positions):
    row_count = queries.shape[0]
    head_count = queries.shape[1] // QKD
    normed = head_norm(queries.astype(jnp.float32).reshape(row_count, head_count, QKD), query_gain)
    turned = jnp.concatenate(
        [normed[..., :NOPE], rotate_half(normed[..., NOPE:], positions)], axis=-1
    )
    return turned.astype(jnp.bfloat16)


def make_keys(latent, rope_part, latent_gain, key_up, value_up, key_gain, positions):
    row_count = latent.shape[0]
    head_count = key_up.shape[1] // NOPE
    latent_f = latent.astype(jnp.float32)
    latent_n = (
        latent_f
        * lax.rsqrt(jnp.mean(latent_f * latent_f, axis=-1, keepdims=True) + EPS)
        * latent_gain
    ).astype(jnp.bfloat16)
    key_nope = jnp.dot(latent_n, key_up, preferred_element_type=jnp.float32).astype(jnp.bfloat16)
    key_nope = lax.optimization_barrier(key_nope)
    value_rows = jnp.dot(latent_n, value_up, preferred_element_type=jnp.float32).astype(
        jnp.bfloat16
    )
    shared = jnp.broadcast_to(
        rope_part.astype(jnp.float32)[:, None, :], (row_count, head_count, ROPE)
    )
    key_full = jnp.concatenate(
        [key_nope.astype(jnp.float32).reshape(row_count, head_count, NOPE), shared], axis=-1
    )
    normed = head_norm(key_full, key_gain)
    turned = jnp.concatenate(
        [normed[..., :NOPE], rotate_half(normed[..., NOPE:], positions)], axis=-1
    )
    return (turned.astype(jnp.bfloat16), value_rows.reshape(row_count, head_count, VDIM))


def shards(
    queries,
    kv_latent,
    rope_key,
    latent_gain,
    key_up,
    value_up,
    query_gain,
    key_gain,
    out_gain,
    out_proj,
    moe_input,
    moe_gain,
    expert_ids,
    route_weights,
    w_gate,
    w_up,
    w_down,
):
    tok_rows = queries.shape[0]
    head_count = key_up.shape[1] // NOPE
    query_pos = lax.axis_index("ep") * tok_rows + jnp.arange(tok_rows, dtype=jnp.int32)
    query_rot = make_queries(queries, query_gain, query_pos)
    inv_scale = QKD ** (-0.5)
    blocks_in = (
        lax.all_gather(kv_latent, "ep", axis=0, tiled=True),
        lax.all_gather(rope_key, "ep", axis=0, tiled=True),
    )
    key_pos = jnp.arange(blocks_in[0].shape[0], dtype=jnp.int32)
    key_rot, value_rows = make_keys(
        blocks_in[0], blocks_in[1], latent_gain, key_up, value_up, key_gain, key_pos
    )
    top_prev = jnp.full((head_count, tok_rows), -1e30, jnp.float32)
    key_pos = jnp.arange(key_rot.shape[0], dtype=jnp.int32)
    scores = (
        jnp.einsum("qhd,khd->hqk", query_rot, key_rot, preferred_element_type=jnp.float32)
        * inv_scale
    )
    visible = key_pos[None, :] <= query_pos[:, None]
    scores = jnp.where(visible[None], scores, -1e30)
    top_new = jnp.maximum(top_prev, jnp.max(scores, axis=-1))
    expo = jnp.exp(scores - top_new[..., None])
    total_new = jnp.sum(expo, axis=-1)
    accum_new = jnp.einsum(
        "hqk,khd->hqd", expo.astype(jnp.bfloat16), value_rows, preferred_element_type=jnp.float32
    )
    attn = (accum_new / total_new[..., None]).astype(jnp.bfloat16)
    attn = attn.transpose(1, 0, 2).reshape(tok_rows, head_count * VDIM)
    block_f = lax.all_gather(attn, "tp", axis=1, tiled=True).astype(jnp.float32)
    scaled = (block_f * out_gain[None, :]).astype(jnp.bfloat16)
    product = jnp.dot(scaled, out_proj, preferred_element_type=jnp.float32)
    product, squares = (product, jnp.sum(block_f * block_f, axis=-1))
    mixed = (product * lax.rsqrt(squares / out_gain.shape[0] + EPS)[:, None]).astype(jnp.bfloat16)
    row_count = moe_input.shape[0]
    top_count = expert_ids.shape[1]
    local_experts = w_gate.shape[0]
    ep_count = lax.axis_size("ep")
    expert_count = local_experts * ep_count
    stream_f = moe_input.astype(jnp.float32)
    normed = (
        stream_f * lax.rsqrt(jnp.mean(stream_f * stream_f, axis=-1, keepdims=True) + EPS) * moe_gain
    ).astype(jnp.bfloat16)
    flat_ids = expert_ids.reshape(-1)
    onehot = (flat_ids[:, None] == jnp.arange(expert_count, dtype=jnp.int32)[None, :]).astype(
        jnp.int32
    )
    slot_rank = jnp.sum((jnp.cumsum(onehot, axis=0) - onehot) * onehot, axis=1)
    slot_index = flat_ids * CAP + slot_rank
    token_index = jnp.arange(row_count * top_count, dtype=jnp.int32) // top_count
    slot_token = jnp.zeros((expert_count * CAP,), jnp.int32).at[slot_index].set(token_index)
    slot_used = jnp.zeros((expert_count * CAP,), jnp.bool_).at[slot_index].set(True)
    outgoing = jnp.where(slot_used[:, None], normed[slot_token], jnp.zeros((), jnp.bfloat16))
    outgoing = outgoing.reshape(ep_count, local_experts, CAP, normed.shape[1])
    piece_width = normed.shape[1] // lax.axis_size("tp")
    my_columns = lax.dynamic_slice_in_dim(
        outgoing, lax.axis_index("tp") * piece_width, piece_width, 3
    )
    arrived_part = lax.all_to_all(my_columns, "ep", split_axis=0, concat_axis=0, tiled=True)
    piece = lax.all_gather(arrived_part, "tp", axis=3, tiled=True)
    gate_acc = jnp.einsum("secd,edf->secf", piece, w_gate, preferred_element_type=jnp.float32)
    upper_acc = jnp.einsum("secd,edf->secf", piece, w_up, preferred_element_type=jnp.float32)
    hidden = (jax.nn.silu(gate_acc) * upper_acc).astype(jnp.bfloat16)
    out_cols = w_down.shape[2] // lax.axis_size("tp")
    term = jnp.einsum("secf,efd->dsec", hidden, w_down, preferred_element_type=jnp.float32)
    summed = lax.psum_scatter(
        term.reshape(lax.axis_size("tp") * out_cols, -1).astype(jnp.bfloat16),
        "tp",
        scatter_dimension=0,
        tiled=True,
    )
    expert_y = summed.T.reshape(ep_count, local_experts * CAP, out_cols)
    returned_rows = lax.all_to_all(expert_y, "ep", split_axis=0, concat_axis=0, tiled=True).reshape(
        expert_count * CAP, out_cols
    )
    picked = returned_rows[slot_index].reshape(row_count, top_count, out_cols).astype(jnp.float32)
    expert_out = jnp.sum(picked * route_weights[..., None], axis=1).astype(jnp.bfloat16)
    return (mixed, expert_out)


MESH = pl.DeviceIdType.MESH
GROUP = 8
PAD = 128


def group_cap():
    return GROUP * CAP // 2


def rdma(src, dst, send_sem, recv_sem, device):
    copy = pltpu.make_async_remote_copy(
        src_ref=src,
        dst_ref=dst,
        send_sem=send_sem,
        recv_sem=recv_sem,
        device_id=device,
        device_id_type=MESH,
    )
    copy.start()
    return copy


def arrived(dst, sem, device):
    pltpu.make_async_remote_copy(
        src_ref=dst,
        dst_ref=dst,
        send_sem=sem,
        recv_sem=sem,
        device_id=device,
        device_id_type=MESH,
    ).wait_recv()


def places(planes):
    ep = lax.axis_index("ep")
    tp = lax.axis_index("tp")
    plane = ep // 2
    core = ep % 2

    def along(offset):
        return (lax.rem(plane + offset + planes, planes) * 2 + core, tp)

    partner = (plane * 2 + 1 - core, tp)
    near_x = (ep, tp ^ 1)
    near_y = (ep, tp ^ 2)
    corner = (ep, tp ^ 3)
    return tp, along, partner, near_x, near_y, corner


def greet(peers):
    barrier = pltpu.get_barrier_semaphore()
    for peer in peers:
        pl.semaphore_signal(barrier, inc=1, device_id=peer, device_id_type=MESH)
    pl.semaphore_wait(barrier, len(peers))


def routed_kernel(
    planes,
    out_ref,
    meta_ref,
    kv_ref,
    gate_ref,
    up_ref,
    down_ref,
    part_ref,
    keys_ref,
    rows_ref,
    metas_ref,
    gates,
    ups,
    downs,
    taken,
    given,
    ws,
    zs,
    zr,
    xs,
    xr,
    ps,
    pr,
    loc,
):
    tp, along, partner, near_x, near_y, _ = places(planes)
    greet([along(d) for d in range(1, planes)] + [partner, near_x, near_y])
    half_w = out_ref.shape[2] // 2
    half_r = kv_ref.shape[0] // 2
    sent = []
    local = [
        pltpu.make_async_copy(kv_ref, keys_ref.at[tp, 0, 0], loc.at[0]),
        pltpu.make_async_copy(meta_ref.at[0], metas_ref.at[0, 0], loc.at[1]),
        pltpu.make_async_copy(out_ref.at[0], rows_ref.at[tp, 0, 0], loc.at[2]),
    ]
    for copy in local:
        copy.start()
    order = sorted(range(1, planes), key=lambda d: (min(d, planes - d), d))
    for d in order:
        sent.append(
            rdma(meta_ref.at[d], metas_ref.at[0, d], zs.at[1, d], zr.at[1, d], along(d))
        )
        sent.append(
            rdma(out_ref.at[d], rows_ref.at[tp, 0, d], zs.at[2, d], zr.at[2, d], along(d))
        )
    for d in order:
        sent.append(rdma(kv_ref, keys_ref.at[tp, 0, d], zs.at[0, d], zr.at[0, d], along(d)))
    experts = gate_ref.shape[0]
    down_slots = downs.shape[0]

    def fetch(which, source, target, expert):
        return pltpu.make_async_copy(source, target, ws.at[which, expert])

    gate_in = [fetch(0, gate_ref.at[e], gates.at[e], e) for e in range(experts)]
    up_in = [fetch(1, up_ref.at[e], ups.at[e], e) for e in range(experts)]
    down_in = [fetch(2, down_ref.at[e], downs.at[e % down_slots], e) for e in range(experts)]
    for e in range(experts):
        gate_in[e].start()
        up_in[e].start()
        if e < down_slots:
            down_in[e].start()
    for copy in local:
        copy.wait()
    bufs = (keys_ref, rows_ref)

    def halves(kind, ref):
        if kind == 0:
            return ref.at[pl.ds(0, half_r)], ref.at[pl.ds(half_r, half_r)]
        return ref.at[:, pl.ds(0, half_w)], ref.at[:, pl.ds(half_w, half_w)]

    def to_partner(kind, which, q, d):
        sent.append(
            rdma(
                bufs[kind].at[q, 0, d],
                bufs[kind].at[q, 1, d],
                ps.at[kind, which, d],
                pr.at[kind, which, d],
                partner,
            )
        )

    def first(kind, d):
        mine = bufs[kind].at[tp, 0, d]
        if d > 0:
            arrived(mine, zr.at[2 * kind, d], along(-d))
        sent.append(rdma(mine, mine, xs.at[kind, 0, d], xr.at[kind, 0, d], near_x))
        sent.append(rdma(mine, mine, xs.at[kind, 1, d], xr.at[kind, 1, d], near_y))
        to_partner(kind, 0, tp, d)
        if kind == 1:
            part = metas_ref.at[0, d]
            if d > 0:
                arrived(part, zr.at[1, d], along(-d))
            sent.append(rdma(part, metas_ref.at[1, d], ps.at[2, 0, d], pr.at[2, 0, d], partner))

    def second(kind, d):
        from_x = bufs[kind].at[tp ^ 1, 0, d]
        arrived(from_x, xr.at[kind, 0, d], near_x)
        low, _ = halves(kind, from_x)
        sent.append(rdma(low, low, xs.at[kind, 2, d], xr.at[kind, 2, d], near_y))
        from_y = bufs[kind].at[tp ^ 2, 0, d]
        arrived(from_y, xr.at[kind, 1, d], near_y)
        _, high = halves(kind, from_y)
        sent.append(rdma(high, high, xs.at[kind, 3, d], xr.at[kind, 3, d], near_x))
        to_partner(kind, 1, tp ^ 1, d)
        to_partner(kind, 2, tp ^ 2, d)

    def third(kind, d):
        low, high = halves(kind, bufs[kind].at[tp ^ 3, 0, d])
        arrived(low, xr.at[kind, 2, d], near_y)
        arrived(high, xr.at[kind, 3, d], near_x)
        to_partner(kind, 3, tp ^ 3, d)

    jobs = [(1, 0), (0, 0)] + [(1, d) for d in order] + [(0, d) for d in order]
    for step in range(len(jobs) + 4):
        if step < len(jobs):
            first(*jobs[step])
        if 0 <= step - 2 < len(jobs):
            second(*jobs[step - 2])
        if 0 <= step - 4 < len(jobs):
            third(*jobs[step - 4])
    for d in range(planes):
        for kind in range(2):
            for which, flip in enumerate((0, 1, 2, 3)):
                arrived(bufs[kind].at[tp ^ flip, 1, d], pr.at[kind, which, d], partner)
        arrived(metas_ref.at[1, d], pr.at[2, 0, d], partner)

    f32, bf = jnp.float32, jnp.bfloat16
    core = lax.axis_index("ep") % 2
    parts, width = part_ref.shape[1], part_ref.shape[3]
    cap = out_ref.shape[1]
    blocks = 2 * planes
    row_total, slots = blocks * cap, blocks * CAP
    info = metas_ref[...].reshape(row_total, PAD)
    codes = info.astype(f32)
    block_of = lax.broadcasted_iota(jnp.int32, (blocks, cap, 1), 0).reshape(row_total, 1)
    slot_ids = lax.broadcasted_iota(jnp.int32, (row_total, experts * slots), 1)
    match = []
    for pick in range(2):
        code = codes[:, pick : pick + 1].astype(jnp.int32) - 1 - core * (experts * CAP)
        inside = (codes[:, pick : pick + 1] > 0.5) & (code >= 0) & (code < experts * CAP)
        expert = jnp.zeros_like(code)
        for e in range(1, experts):
            expert += (code >= e * CAP).astype(jnp.int32)
        where = expert * (slots - CAP) + block_of * CAP + code
        match.append((slot_ids == jnp.where(inside, where, -1)).astype(f32).astype(bf))
    place = match[0] + match[1]
    turned = (((0,), (0,)), ((), ()))
    weights = jnp.zeros((experts * slots, 1), f32)
    for pick in range(2):
        found = lax.dot_general(match[pick], info, turned, preferred_element_type=f32)
        weights += found[:, 2 + pick : 3 + pick] + found[:, 4 + pick : 5 + pick]
    for q in range(parts):
        rows = rows_ref[q].reshape(row_total, width)
        taken[:, q * width : (q + 1) * width] = lax.dot_general(
            place, rows, turned, preferred_element_type=f32
        ).astype(bf)
    for e in range(experts):
        first_slot = e * slots
        picked = taken[first_slot : first_slot + slots, :]
        gate_in[e].wait()
        gate = jnp.dot(picked, gates[e], preferred_element_type=f32)
        up_in[e].wait()
        upper = jnp.dot(picked, ups[e], preferred_element_type=f32)
        hidden = (
            gate / (1.0 + jnp.exp(-gate)) * upper * weights[first_slot : first_slot + slots]
        ).astype(bf)
        down_in[e].wait()
        for q in range(parts):
            given[first_slot : first_slot + slots, q * width : (q + 1) * width] = jnp.dot(
                hidden,
                downs[e % down_slots, :, q * width : (q + 1) * width],
                preferred_element_type=f32,
            ).astype(bf)
        if e + down_slots < experts:
            down_in[e + down_slots].start()
    for q in range(parts):
        back = jnp.dot(
            place, given[:, q * width : (q + 1) * width], preferred_element_type=f32
        )
        part_ref[:, q] = back.astype(bf).reshape(blocks, cap, width)
    for copy in sent:
        copy.wait_send()


def routed(outgoing, metas, kv_part, w_gate, w_up, w_down, tp_count):
    planes, cap, width = outgoing.shape
    experts, model, hidden = w_gate.shape
    blocks = 2 * planes
    slot_total = experts * blocks * CAP
    dma = pltpu.SemaphoreType.DMA
    bf = jnp.bfloat16
    vmem = pl.BlockSpec(memory_space=pltpu.VMEM)
    hbm = pl.BlockSpec(memory_space=pl.ANY)
    return pl.pallas_call(
        functools.partial(routed_kernel, planes),
        out_shape=(
            jax.ShapeDtypeStruct((blocks, tp_count, cap, width), bf),
            jax.ShapeDtypeStruct((tp_count, 2, planes) + kv_part.shape, bf),
        ),
        in_specs=[vmem] * 3 + [hbm] * 3,
        out_specs=(vmem,) * 2,
        scratch_shapes=[
            pltpu.VMEM((tp_count, 2, planes, cap, width), bf),
            pltpu.VMEM((2, planes, cap, PAD), bf),
            pltpu.VMEM((experts, model, hidden), bf),
            pltpu.VMEM((experts, model, hidden), bf),
            pltpu.VMEM((2, hidden, model), bf),
            pltpu.VMEM((slot_total, model), bf),
            pltpu.VMEM((slot_total, model), bf),
            dma((3, experts)),
            dma((3, planes)),
            dma((3, planes)),
            dma((2, 4, planes)),
            dma((2, 4, planes)),
            dma((3, 4, planes)),
            dma((3, 4, planes)),
            dma((3,)),
        ],
        compiler_params=pltpu.CompilerParams(
            collective_id=0, has_side_effects=True, vmem_limit_bytes=67043328
        ),
        name="routed",
    )(outgoing, metas, kv_part, w_gate, w_up, w_down)


def combine_kernel(
    planes,
    part_ref,
    attn_ref,
    back_ref,
    heads_ref,
    other,
    sums,
    bx1,
    by1,
    bx2,
    by2,
    done,
    as_,
    ar,
    ps,
    pr,
    xs,
    xr,
    zs,
    zr,
    loc,
):
    tp, along, partner, near_x, near_y, corner = places(planes)
    greet([along(d) for d in range(1, planes)] + [partner, near_x, near_y, corner])
    half_w = part_ref.shape[4] // 2
    low, high = pl.ds(0, half_w), pl.ds(half_w, half_w)
    sent = []
    order = list(range(1, planes)) + [0]
    for d in order:
        sent.append(rdma(part_ref.at[1, d], other.at[d], ps.at[d], pr.at[d], partner))
    own = pltpu.make_async_copy(attn_ref, heads_ref.at[tp], loc.at[0])
    own.start()
    for i, peer in enumerate((near_x, near_y, corner)):
        sent.append(rdma(attn_ref, heads_ref.at[tp], as_.at[i], ar.at[i], peer))

    def first(d):
        arrived(other.at[d], pr.at[d], partner)
        for q in range(part_ref.shape[2]):
            sums[d, q] = (
                part_ref[0, d, q].astype(jnp.float32) + other[d, q].astype(jnp.float32)
            ).astype(jnp.bfloat16)
        piece = sums.at[d, tp ^ 3]
        sent.append(rdma(piece.at[:, low], bx1.at[d], xs.at[0, d], xr.at[0, d], near_x))
        sent.append(rdma(piece.at[:, high], by1.at[d], xs.at[1, d], xr.at[1, d], near_y))

    def second(d):
        arrived(bx1.at[d], xr.at[0, d], near_x)
        sums[d, tp ^ 2, :, low] = (
            sums[d, tp ^ 2, :, low].astype(jnp.float32) + bx1[d].astype(jnp.float32)
        ).astype(jnp.bfloat16)
        sent.append(rdma(sums.at[d, tp ^ 2], by2.at[d], xs.at[3, d], xr.at[3, d], near_y))
        arrived(by1.at[d], xr.at[1, d], near_y)
        sums[d, tp ^ 1, :, high] = (
            sums[d, tp ^ 1, :, high].astype(jnp.float32) + by1[d].astype(jnp.float32)
        ).astype(jnp.bfloat16)
        sent.append(rdma(sums.at[d, tp ^ 1], bx2.at[d], xs.at[2, d], xr.at[2, d], near_x))

    def third(d):
        arrived(bx2.at[d], xr.at[2, d], near_x)
        arrived(by2.at[d], xr.at[3, d], near_y)
        full = (
            sums[d, tp].astype(jnp.float32)
            + bx2[d].astype(jnp.float32)
            + by2[d].astype(jnp.float32)
        ).astype(jnp.bfloat16)
        if d == 0:
            back_ref[0] = full
        else:
            done[d] = full
            sent.append(rdma(done.at[d], back_ref.at[d], zs.at[d], zr.at[d], along(-d)))

    for step in range(planes + 2):
        if step < planes:
            first(order[step])
        if 0 <= step - 1 < planes:
            second(order[step - 1])
        if 0 <= step - 2 < planes:
            third(order[step - 2])
    own.wait()
    for i, peer in enumerate((near_x, near_y, corner)):
        arrived(heads_ref.at[tp ^ (i + 1)], ar.at[i], peer)
    for d in range(1, planes):
        arrived(back_ref.at[d], zr.at[d], along(d))
    for copy in sent:
        copy.wait_send()


def combine(parts, attn):
    _, planes, tp_count, cap, width = parts.shape
    dma = pltpu.SemaphoreType.DMA
    bf = jnp.bfloat16
    return pl.pallas_call(
        functools.partial(combine_kernel, planes),
        out_shape=(
            jax.ShapeDtypeStruct((planes, cap, width), bf),
            jax.ShapeDtypeStruct((tp_count,) + attn.shape, bf),
        ),
        in_specs=[pl.BlockSpec(memory_space=pltpu.VMEM)] * 2,
        out_specs=(pl.BlockSpec(memory_space=pltpu.VMEM),) * 2,
        scratch_shapes=[
            pltpu.VMEM((planes, tp_count, cap, width), bf),
            pltpu.VMEM((planes, tp_count, cap, width), bf),
            pltpu.VMEM((planes, cap, width // 2), bf),
            pltpu.VMEM((planes, cap, width // 2), bf),
            pltpu.VMEM((planes, cap, width), bf),
            pltpu.VMEM((planes, cap, width), bf),
            pltpu.VMEM((planes, cap, width), bf),
            dma((3,)),
            dma((3,)),
            dma((planes,)),
            dma((planes,)),
            dma((4, planes)),
            dma((4, planes)),
            dma((planes,)),
            dma((planes,)),
            dma((1,)),
        ],
        compiler_params=pltpu.CompilerParams(
            collective_id=1, has_side_effects=True, vmem_limit_bytes=40 * 2**20
        ),
        name="combine",
    )(parts, attn)


def grouped_shards(
    queries,
    kv_latent,
    rope_key,
    latent_gain,
    key_up,
    value_up,
    query_gain,
    key_gain,
    out_gain,
    out_proj,
    moe_input,
    moe_gain,
    expert_ids,
    route_weights,
    w_gate,
    w_up,
    w_down,
):
    f32, bf = jnp.float32, jnp.bfloat16
    ep, tp = lax.axis_index("ep"), lax.axis_index("tp")
    tp_count = lax.axis_size("tp")
    planes = lax.axis_size("ep") // 2
    plane, core = ep // 2, ep % 2
    tokens, model = moe_input.shape
    width = model // tp_count
    cap = group_cap()

    group = expert_ids[:, 0] // GROUP
    offset = lax.rem(group - plane + planes, planes)
    before = (jnp.arange(tokens)[:, None] > jnp.arange(tokens)[None, :]).astype(bf)
    in_group = offset[:, None] == jnp.arange(planes)[None, :]
    local_ids = expert_ids % GROUP
    hit = [offset[:, None] * GROUP + local_ids[:, k : k + 1] == jnp.arange(planes * GROUP)[None, :] for k in range(2)]
    counted = jnp.concatenate([in_group, hit[0] | hit[1]], axis=1).astype(bf)
    earlier = jnp.dot(before, counted, preferred_element_type=f32)
    rank = jnp.sum(jnp.where(in_group, earlier[:, :planes], 0.0), axis=1).astype(jnp.int32)
    codes = [
        local_ids[:, k].astype(f32) * CAP
        + jnp.sum(jnp.where(hit[k], earlier[:, planes:], 0.0), axis=1)
        + 1.0
        for k in range(2)
    ]
    weight_high = lax.reduce_precision(route_weights, 8, 7)
    weight_low = route_weights - weight_high
    meta = jnp.concatenate(
        [codes[0][:, None], codes[1][:, None], weight_high, weight_low], axis=1
    ).astype(bf)
    meta = jnp.pad(meta, ((0, 0), (0, PAD - meta.shape[1])))
    slot = offset * cap + rank
    select = (jnp.arange(planes * cap)[:, None] == slot[None, :]).astype(bf)

    stream_f = moe_input.astype(f32)
    scale = lax.rsqrt(jnp.mean(stream_f * stream_f, axis=-1, keepdims=True) + EPS)
    own_cols = lax.dynamic_slice_in_dim(moe_input, tp * width, width, 1).astype(f32)
    own_gain = lax.dynamic_slice_in_dim(moe_gain, tp * width, width, 0)
    normed = (own_cols * scale * own_gain).astype(bf)
    outgoing = jnp.dot(select, normed, preferred_element_type=f32).astype(bf)
    metas_out = jnp.dot(select, meta, preferred_element_type=f32).astype(bf)

    kv_rows = kv_latent.shape[0] // tp_count
    kv_all = jnp.pad(
        jnp.concatenate([kv_latent, rope_key], axis=1), ((0, 0), (0, PAD - ROPE))
    )
    kv_part = lax.dynamic_slice_in_dim(kv_all, tp * kv_rows, kv_rows, 0)
    partial, keys = routed(
        outgoing.reshape(planes, cap, width),
        metas_out.reshape(planes, cap, PAD),
        kv_part,
        w_gate,
        w_up,
        w_down,
        tp_count,
    )
    partial = partial.reshape(2, planes, tp_count, cap, width)

    tok_rows = queries.shape[0]
    head_count = key_up.shape[1] // NOPE
    query_pos = ep * tok_rows + jnp.arange(tok_rows, dtype=jnp.int32)
    query_rot = make_queries(queries, query_gain, query_pos)
    latent_width = kv_latent.shape[1]
    key_table = keys.reshape(-1, keys.shape[-1])
    quarter = jnp.arange(tp_count, dtype=jnp.int32)[:, None, None, None]
    parity = jnp.arange(2, dtype=jnp.int32)[None, :, None, None]
    away = jnp.arange(planes, dtype=jnp.int32)[None, None, :, None]
    key_block = lax.rem(plane - away + planes, planes) * 2 + lax.rem(core + parity, 2)
    key_pos = (
        key_block * tok_rows
        + quarter * kv_rows
        + jnp.arange(kv_rows, dtype=jnp.int32)[None, None, None, :]
    ).reshape(-1)
    key_rot, value_rows = make_keys(
        key_table[:, :latent_width],
        key_table[:, latent_width : latent_width + ROPE],
        latent_gain,
        key_up,
        value_up,
        key_gain,
        key_pos,
    )
    scores = (
        jnp.einsum("qhd,khd->hqk", query_rot, key_rot, preferred_element_type=f32) * QKD ** (-0.5)
    )
    visible = key_pos[None, :] <= query_pos[:, None]
    scores = jnp.where(visible[None], scores, -1e30)
    expo = jnp.exp(scores - jnp.max(scores, axis=-1, keepdims=True))
    total = jnp.sum(expo, axis=-1)
    accum = jnp.einsum("hqk,khd->hqd", expo.astype(bf), value_rows, preferred_element_type=f32)
    attn = (accum / total[..., None]).astype(bf)
    attn = attn.transpose(1, 0, 2).reshape(tok_rows, head_count * VDIM)

    returned, heads = combine(partial, attn)

    block_f = heads.transpose(1, 0, 2).reshape(tok_rows, -1).astype(f32)
    scaled = (block_f * out_gain[None, :]).astype(bf)
    product = jnp.dot(scaled, out_proj, preferred_element_type=f32)
    squares = jnp.sum(block_f * block_f, axis=-1)
    mixed = (product * lax.rsqrt(squares / out_gain.shape[0] + EPS)[:, None]).astype(bf)
    expert_out = lax.dot_general(
        select,
        returned.reshape(planes * cap, width),
        (((0,), (0,)), ((), ())),
        preferred_element_type=f32,
    ).astype(bf)
    return (mixed, expert_out)


def layer(*arrays):
    local_experts = arrays[14].shape[0]
    fits = lax.axis_size("tp") == 4 and 2 * local_experts == GROUP
    return grouped_shards(*arrays) if fits else shards(*arrays)


def solution(mesh):
    in_specs = (
        P("ep", "tp"),
        P("ep", None),
        P("ep", None),
        P(),
        P(None, "tp"),
        P(None, "tp"),
        P(),
        P(),
        P(),
        P(None, "tp"),
        P("ep", None),
        P(),
        P("ep", None),
        P("ep", None),
        P("ep", None, "tp"),
        P("ep", None, "tp"),
        P("ep", "tp", None),
    )
    out_specs = (P("ep", "tp"), P("ep", "tp"))
    return jax.shard_map(layer, mesh=mesh, in_specs=in_specs, out_specs=out_specs, check_vma=False)
```
